32 devices in a mesh: grp: 2 (over y), sp: 4 (over z), tp: 4 (over x, core).
Axes of the slice: x: 2, y: 2, z: 4, core: 2. Of those that a mesh axis runs over, the one named last changes fastest.
Arguments:
- tokens: bfloat16 [4096, 2048], P(('grp', 'sp'), 'tp'), parts along dimension 0, may hold values from -140 to 140, as said below
- mix_gain: bfloat16 [2, 2048], replicated, may hold values from 0.099609375 to 1.8984375
- gate_weight: bfloat16 [2, 2048, 2048], P(None, 'sp', 'tp'), may hold values from -0.125 to 0.125
- mix_weight: bfloat16 [2, 2048, 2048], P(None, 'sp', 'tp'), may hold values from -0.125 to 0.125
- value_weight: bfloat16 [2, 2048, 2048], P(None, 'sp', 'tp'), may hold values from -0.125 to 0.125
- out_weight: bfloat16 [2, 2048, 2048], P(None, 'sp', 'tp'), may hold values from -0.125 to 0.125
- conv_taps: bfloat16 [2, 3, 2048], P(None, None, 'tp'), may hold values from -3.5 to 3.5
Outputs:
- result_stream: bfloat16 [4096, 2048], P(('grp', 'sp'), 'tp'), parts along dimension 0
The draws below stay inside these ranges and needn't reach their ends.
There are 2 independent parts, one for each index of `grp`. The reference program is written for one: setup_inputs(seed, part) draws one part's arguments, and reference() takes and returns one part's arrays. A program takes and returns all parts, laid end to end along the dimension named above; an argument that names none is the same for every part. Nothing has to cross between parts.
Inputs may be any that keep to these rules, and one draw needn't show every extreme that they name: `tokens`: activations with feature scales of several sizes.
All inputs are finite; a program needn't handle non-finite values.
Results may differ from the reference program's by a relative error of at most 0.015.
Values may be sent and summed in bfloat16 or wider, within the bound.
A program may use at most 64 MiB of HBM per device.

```python
import jax
import jax.numpy as jnp
from jax import lax

D = 2048
TAPS = 3
LAYERS = 2
TOKENS = 2048


def draw_tokens(key, part):
    subkeys = jax.random.split(key, 2)
    normal_part = jnp.clip(jax.random.normal(subkeys[0], (TOKENS, D), jnp.float32), -6.0, 6.0)
    column = 10.0 ** (jax.random.uniform(subkeys[1], (D,), jnp.float32) - 0.5)
    column = column * 3.0 ** (jnp.arange(D, dtype=jnp.float32) / D - 0.5)
    return (normal_part * column).astype(jnp.bfloat16)


def levels(rng, shape, cuts, least, top_value):
    gain, own = 1.0, jax.random.fold_in(rng, 6)
    for position, parts in cuts:
        draws = jnp.exp(jax.random.uniform(jax.random.fold_in(own, position), (parts,), jnp.float32, least / len(cuts), top_value / len(cuts)))
        gain = gain * jnp.repeat(draws, shape[position] // parts).reshape([-1 if axis == position else 1 for axis in range(len(shape))])
    return gain


def scatter_about(own_key, shape, scale, reach, pieces=(), kind=jnp.bfloat16):
    entries = jax.random.normal(own_key, shape, jnp.float32) * scale
    if len(pieces) > 0:
        entries = levels(own_key, shape, pieces, -0.22, 0.18) * entries
    return jnp.clip(entries, min=-reach, max=reach).astype(kind)


def setup_inputs(seed: int = 0, part: int = 0) -> dict:
    arg_keys = jax.random.split(jax.random.key(seed), 8)
    own_keys = jax.random.split(jax.random.fold_in(arg_keys[7], part), 8)
    tokens = draw_tokens(jax.random.fold_in(jax.random.fold_in(arg_keys[7], part), 71), part)
    mix_gain = jnp.clip(1.0 + 0.18 * jax.random.normal(arg_keys[1], (LAYERS, D), jnp.float32), 0.099609375, 1.8984375).astype(jnp.bfloat16)
    gate_weight = scatter_about(arg_keys[2], (LAYERS, D, D), D ** -0.5, 0.125, ((1, 4), (2, 4)))
    mix_weight = scatter_about(arg_keys[3], (LAYERS, D, D), D ** -0.5, 0.125, ((1, 4), (2, 4)))
    value_weight = scatter_about(arg_keys[4], (LAYERS, D, D), D ** -0.5, 0.125, ((1, 4), (2, 4)))
    out_weight = scatter_about(arg_keys[5], (LAYERS, D, D), D ** -0.5, 0.125, ((1, 4), (2, 4)))
    conv_taps = scatter_about(arg_keys[6], (LAYERS, TAPS, D), TAPS ** -0.5, 3.5, ((2, 4),))
    return {"tokens": tokens, "mix_gain": mix_gain, "gate_weight": gate_weight, "mix_weight": mix_weight, "value_weight": value_weight, "out_weight": out_weight, "conv_taps": conv_taps}


EPS = 1e-06

def reference(tokens, mix_gain, gate_weight, mix_weight, value_weight, out_weight, conv_taps):
    stream = tokens
    for layer_index in range(LAYERS):
        wide_rows = stream.astype(jnp.float32)
        factor = lax.rsqrt(lax.optimization_barrier(jnp.mean(wide_rows * wide_rows, axis=1, keepdims=True)) + EPS)
        normed = (wide_rows * factor * mix_gain[layer_index].astype(jnp.float32)).astype(jnp.bfloat16)
        gate = jnp.dot(normed, gate_weight[layer_index], preferred_element_type=jnp.float32).astype(jnp.bfloat16)
        inner = jnp.dot(normed, mix_weight[layer_index], preferred_element_type=jnp.float32).astype(jnp.bfloat16)
        values = jnp.dot(normed, value_weight[layer_index], preferred_element_type=jnp.float32).astype(jnp.bfloat16)
        carried = inner.astype(jnp.float32) * values.astype(jnp.float32)
        padded = jnp.pad(carried, ((TAPS - 1, 0), (0, 0)))
        row_count = carried.shape[0]
        tap_rows = conv_taps[layer_index].astype(jnp.float32)
        conv = jnp.zeros_like(carried)
        for tap_index in range(TAPS):
            conv = conv + tap_rows[tap_index] * padded[tap_index:tap_index + row_count]
        mixed = (gate.astype(jnp.float32) * conv).astype(jnp.bfloat16)
        product = jnp.dot(mixed, out_weight[layer_index], preferred_element_type=jnp.float32)
        stream = (wide_rows + product).astype(jnp.bfloat16)
    return stream
```

```python
import jax
import jax.numpy as jnp
from jax import lax
from jax.sharding import PartitionSpec as P

EPS = 1e-06


def shifted(x, axis, by):
    n = lax.axis_size(axis)
    return lax.ppermute(x, axis, [(i, (i + by) % n) for i in range(n)])


def swapped(x, axis):
    n = lax.axis_size(axis)
    return lax.ppermute(x, axis, [(i, i ^ 1) for i in range(n)])


def passed_along(x, axis, by):
    n = lax.axis_size(axis)
    return lax.ppermute(x, axis, [(i, i + by) for i in range(n) if 0 <= i + by < n])


def rows_gathered(block):
    n = lax.axis_size("sp")
    me = lax.axis_index("sp")
    depth, width = block.shape
    whole = jnp.zeros((n * depth, width), block.dtype)
    whole = lax.dynamic_update_slice(whole, block, (me * depth, 0))
    from_left, from_right = [block], [block]
    for _ in range(n - 1):
        from_left.append(passed_along(from_left[-1], "sp", 1))
        from_right.append(passed_along(from_right[-1], "sp", -1))
    for step in range(1, n):
        piece = jnp.where(me >= step, from_left[step], from_right[n - step])
        whole = lax.dynamic_update_slice(whole, piece, (lax.rem(me - step + n, n) * depth, 0))
    return whole


def channel_gathered(block, place):
    groups, tps = lax.axis_size("grp"), lax.axis_size("tp")
    lows = 2 if tps % 2 == 0 else 1
    highs = tps // lows
    my_grp, my_tp = lax.axis_index("grp"), lax.axis_index("tp")
    my_high, my_low = my_tp // lows, lax.rem(my_tp, lows)
    half = block.shape[0] // 2
    pieces = {}
    top, bottom = block[:half], block[half:]
    pieces[0, 0] = [(0, top), (half, bottom)]
    line = [block]
    for s in range(1, highs):
        line.append(shifted(line[-1], "tp", lows))
        pieces[0, s] = [(0, line[s])]
    tops = [x[:half] for x in line]
    over = block
    for g in range(1, groups):
        over = shifted(over, "grp", 1)
        pieces[g, 0] = [(0, over)]
        low_half = over[half:]
        tops = [None] + [shifted(x, "grp", 1) for x in tops[1:]]
        for s in range(1, highs):
            low_half = shifted(low_half, "tp", lows)
            pieces[g, s] = [(0, tops[s]), (half, low_half)]
    pieces[0, 0] = [(0, block)]
    found = []
    for (g, s), parts in pieces.items():
        origin_grp = lax.rem(my_grp - g + groups, groups)
        origin_high = lax.rem(my_high - s + highs, highs)
        for offset, part in parts:
            found.append((origin_grp, origin_high * lows + my_low, offset, part))
            if lows == 2:
                found.append((origin_grp, origin_high * lows + 1 - my_low, offset, swapped(part, "tp")))
    return [(place(g, t), offset, part) for g, t, offset, part in found]


def assembled(found, shape, dtype):
    whole = jnp.zeros(shape, dtype)
    for (row, column), offset, part in found:
        whole = lax.dynamic_update_slice(whole, part, (row + offset, column))
    return whole


def shards(tokens, mix_gain, gate_weight, mix_weight, value_weight, out_weight, conv_taps):
    groups, tps = lax.axis_size("grp"), lax.axis_size("tp")
    my_grp, my_tp = lax.axis_index("grp"), lax.axis_index("tp")
    layer_count, _, block_width = gate_weight.shape
    width = block_width // groups
    rows = tokens.shape[0]
    features = tps * block_width
    reach = conv_taps.shape[1] - 1

    def mine(w):
        return lax.dynamic_slice_in_dim(w, my_grp * width, width, axis=w.ndim - 1)

    inputs, outs = [], []
    for layer in range(layer_count):
        stacked = jnp.concatenate(
            [mine(gate_weight[layer]), mine(mix_weight[layer]), mine(value_weight[layer])], axis=1
        )
        inputs.append(rows_gathered(stacked))
        outs.append(rows_gathered(mine(out_weight[layer])))
    taps = mine(conv_taps).astype(jnp.float32)

    shape = (groups * rows, features)
    column_place = lambda g, t: (0, t * block_width + g * width)
    found = channel_gathered(tokens, lambda g, t: (g * rows, t * block_width))
    stream = None
    for layer in range(layer_count):
        whole = assembled(found, shape, tokens.dtype)
        if stream is None:
            stream = lax.dynamic_slice(whole, (0, my_tp * block_width + my_grp * width), (shape[0], width))
        wide = whole.astype(jnp.float32)
        factor = lax.rsqrt(jnp.mean(wide * wide, axis=1, keepdims=True) + EPS)
        normed = (wide * factor * mix_gain[layer].astype(jnp.float32)).astype(jnp.bfloat16)
        projected = jnp.dot(normed, inputs[layer], preferred_element_type=jnp.float32).astype(jnp.bfloat16)
        gate, inner, values = (projected[:, k * width : (k + 1) * width].astype(jnp.float32) for k in range(3))
        carried = (inner * values).reshape(groups, rows, width)
        before = passed_along(carried[:, rows - reach :], "sp", 1)
        padded = jnp.concatenate([before, carried], axis=1)
        conv = jnp.zeros_like(carried)
        for tap in range(reach + 1):
            conv = conv + taps[layer, tap] * padded[:, tap : tap + rows]
        mixed = (gate * conv.reshape(groups * rows, width)).astype(jnp.bfloat16)
        mixed_all = assembled(channel_gathered(mixed, column_place), shape, mixed.dtype)
        product = jnp.dot(mixed_all, outs[layer], preferred_element_type=jnp.float32)
        stream = (stream.astype(jnp.float32) + product).astype(jnp.bfloat16)
        if layer < layer_count - 1:
            found = channel_gathered(stream, column_place)
    result = jnp.zeros((rows, block_width), stream.dtype)
    for g in range(groups):
        rows_for = lax.rem(my_grp + g, groups)
        piece = lax.dynamic_slice_in_dim(stream, rows_for * rows, rows, axis=0)
        if g > 0:
            piece = shifted(piece, "grp", g)
        source = lax.rem(my_grp - g + groups, groups)
        result = lax.dynamic_update_slice(result, piece, (0, source * width))
    return result


def solution(mesh):
    return jax.shard_map(
        shards,
        mesh=mesh,
        in_specs=(
            P(("grp", "sp"), "tp"),
            P(),
            P(None, "sp", "tp"),
            P(None, "sp", "tp"),
            P(None, "sp", "tp"),
            P(None, "sp", "tp"),
            P(None, None, "tp"),
        ),
        out_specs=P(("grp", "sp"), "tp"),
        check_vma=False,
    )
```

```python
import functools

import jax
import jax.numpy as jnp
from jax import lax
from jax.experimental import pallas as pl
from jax.experimental.pallas import tpu as pltpu
from jax.sharding import PartitionSpec as P

EPS = 1e-06
KINDS = 4
MESH = pl.DeviceIdType.MESH


def kernel(sizes, tokens, gain, gate_w, mix_w, value_w, out_w, taps, result,
           wide, acts, carried, gates, edge_out, edge_in, last, swap_in,
           local_sem, w_send, w_recv, a_send, a_recv, e_send, e_recv, r_send, r_recv):
    groups, n, tps, lows = sizes
    highs = tps // lows
    rows, block_width = tokens.shape
    layers = gate_w.shape[0]
    depth = gate_w.shape[1]
    width = block_width // groups
    all_rows = groups * rows
    reach = edge_in.shape[2]
    chunk = min(rows, 256)
    me, my_grp, my_tp = lax.axis_index("sp"), lax.axis_index("grp"), lax.axis_index("tp")
    my_high, my_low = my_tp // lows, lax.rem(my_tp, lows)

    def tp_at(high, low):
        return lax.rem(high + highs, highs) * lows + low

    x_next, x_prev = {"tp": tp_at(my_high + 1, my_low)}, {"tp": tp_at(my_high - 1 + highs, my_low)}
    across = {"grp": lax.rem(my_grp + 1, groups)}
    sibling = {"tp": my_high * lows + (1 - my_low)}
    right, left = {"sp": me + 1}, {"sp": me - 1}

    barrier = pltpu.get_barrier_semaphore()
    fixed = []
    if highs > 1:
        fixed.append(x_next)
    if highs > 2:
        fixed.append(x_prev)
    if groups > 1:
        fixed.append(across)
    if lows > 1:
        fixed.append(sibling)
    for device in fixed:
        pl.semaphore_signal(barrier, inc=1, device_id=device, device_id_type=MESH)

    @pl.when(me > 0)
    def _():
        pl.semaphore_signal(barrier, inc=1, device_id=left, device_id_type=MESH)

    @pl.when(me < n - 1)
    def _():
        pl.semaphore_signal(barrier, inc=1, device_id=right, device_id_type=MESH)

    weights = (gate_w, mix_w, value_w, out_w)
    own_columns = pl.ds(pl.multiple_of(my_grp * width, width), width)

    def w_rows(origin):
        return pl.ds(pl.multiple_of(origin * depth, depth), depth)

    def token_place(g, t, offset, size):
        return (pl.ds(pl.multiple_of(g * rows + offset, size), size),
                pl.ds(pl.multiple_of(t * block_width, block_width), block_width))

    def column_place(g, t, offset, size):
        return (pl.ds(offset, size), pl.ds(pl.multiple_of(t * block_width + g * width, width), width))

    own = column_place(my_grp, my_tp, 0, all_rows)[1]
    locals_ = [pltpu.make_async_copy(tokens, acts.at[(0,) + token_place(my_grp, my_tp, 0, rows)], local_sem.at[0])]
    for m in range(layers * KINDS):
        locals_.append(pltpu.make_async_copy(
            weights[m % KINDS].at[m // KINDS, :, own_columns], wide.at[m, w_rows(me), :], local_sem.at[m + 1]))
    for copy in locals_:
        copy.start()
    for copy in locals_:
        copy.wait()

    pl.semaphore_wait(barrier, len(fixed) + jnp.minimum(me, 1) + jnp.minimum(n - 1 - me, 1))

    def w_copy(m, origin, way):
        ref = wide.at[m, w_rows(origin), :]
        return pltpu.make_async_remote_copy(
            src_ref=ref, dst_ref=ref, send_sem=w_send.at[m, way, origin], recv_sem=w_recv.at[m, origin],
            device_id=right if way == 0 else left, device_id_type=MESH)

    def w_own(m):
        @pl.when(me < n - 1)
        def _():
            w_copy(m, me, 0).start()

        @pl.when(me > 0)
        def _():
            w_copy(m, me, 1).start()

    def w_event(m, k):
        @pl.when(me - k >= 0)
        def _():
            w_copy(m, me - k, 0).wait_recv()

            @pl.when(me < n - 1)
            def _():
                w_copy(m, me - k, 0).start()

        @pl.when(me + k < n)
        def _():
            w_copy(m, me + k, 1).wait_recv()

            @pl.when(me > 0)
            def _():
                w_copy(m, me + k, 1).start()

    queue = []
    total = layers * KINDS
    ahead = min(3, total)
    lead = 2 * (n - 1)
    for first in range(0, total, KINDS):
        for part in ((0, 1, 2), (3,)):
            for k in range(1, n):
                for j in part:
                    queue.append((first + j, k))
    state = {"issued": ahead, "done": 0}

    def serve(count):
        while count > 0 and state["done"] < len(queue):
            m, k = queue[state["done"]]
            w_event(m, k)
            state["done"] += 1
            count -= 1
            while state["issued"] < total and queue.index((state["issued"], 1)) <= state["done"] + lead:
                w_own(state["issued"])
                state["issued"] += 1

    def serve_until(m):
        while any(q[0] == m for q in queue[state["done"]:]):
            serve(1)

    sends = []

    def gather(index, place, full, per):
        half = full // 2
        lane = {"next": 0}

        def copy(origin_grp, origin_tp, offset, size, device, slot):
            ref = acts.at[(index,) + place(origin_grp, origin_tp, offset, size)]
            return pltpu.make_async_remote_copy(
                src_ref=ref, dst_ref=ref, send_sem=a_send.at[index, slot], recv_sem=a_recv.at[index, slot],
                device_id=device, device_id_type=MESH)

        def send(g, s, offset, size, device, slot):
            c = copy(lax.rem(my_grp + g, groups), tp_at(my_high - s + highs, my_low), offset, size, device, slot)
            c.start()
            sends.append(c)

        def arrived(g, s, offset, size, slot, low=None):
            low = my_low if low is None else low
            copy(lax.rem(my_grp + g, groups), tp_at(my_high - s + highs, low), offset, size, x_next, slot).wait_recv()

        def to_sibling(g, s, offset, size):
            if lows > 1:
                slot = lane["next"]
                lane["next"] += 1
                send(g, s, offset, size, sibling, slot)
                expected.append((g, s, offset, size, slot))

        expected = []
        base = 5 * highs
        x_slot, y_slot = base, base + highs
        top_slot, low_slot = y_slot + 1, y_slot + 1 + highs
        if highs > 1:
            send(0, 0, 0, full, x_next, x_slot)
        if groups > 1:
            send(0, 0, 0, full, across, y_slot)
        to_sibling(0, 0, 0, full)
        serve(per[0])
        for s in range(1, highs):
            arrived(0, s, 0, full, x_slot + s - 1)
            if groups > 1:
                send(0, s, 0, half, across, top_slot + s - 1)
            if s < highs - 1:
                send(0, s, 0, full, x_next, x_slot + s)
            to_sibling(0, s, 0, full)
        if groups > 1:
            arrived(1, 0, 0, full, y_slot)
            if highs > 1:
                send(1, 0, half, half, x_next, low_slot)
            to_sibling(1, 0, 0, full)
            serve(per[1])
            for s in range(1, highs):
                arrived(1, s, half, half, low_slot + s - 1)
                if s < highs - 1:
                    send(1, s, half, half, x_next, low_slot + s)
                to_sibling(1, s, half, half)
                arrived(1, s, 0, half, top_slot + s - 1)
                to_sibling(1, s, 0, half)
        for g, s, offset, size, slot in expected:
            arrived(g, s, offset, size, slot, 1 - my_low)

    for m in range(ahead):
        w_own(m)
    gather(0, token_place, rows, (2, 1))

    for layer in range(layers):
        now, mixed_at = 2 * layer, 2 * layer + 1
        first = layer * KINDS
        for j in range(3):
            serve_until(first + j)

        def project(g, c):
            start = g * rows + c * chunk
            picked = pl.ds(pl.multiple_of(start, chunk), chunk)
            x = acts[now, picked, :].astype(jnp.float32)
            factor = lax.rsqrt(jnp.mean(x * x, axis=1, keepdims=True) + EPS)
            normed = (x * factor * gain[layer : layer + 1, :].astype(jnp.float32)).astype(jnp.bfloat16)
            gates[picked, :] = jnp.dot(normed, wide[first], preferred_element_type=jnp.float32).astype(jnp.bfloat16)
            inner = jnp.dot(normed, wide[first + 1], preferred_element_type=jnp.float32).astype(jnp.bfloat16)
            values = jnp.dot(normed, wide[first + 2], preferred_element_type=jnp.float32).astype(jnp.bfloat16)
            carried[g, pl.ds(pl.multiple_of(8 + c * chunk, 8), chunk), :] = (
                inner.astype(jnp.float32) * values.astype(jnp.float32))

        chunks = rows // chunk

        @pl.loop(0, groups * chunks)
        def _(i):
            project(lax.rem(i, groups), chunks - 1 - i // groups)

        for g in range(groups):
            edge_out[layer, g] = carried[g, 8 + rows - reach : 8 + rows, :]
        edge = pltpu.make_async_remote_copy(
            src_ref=edge_out.at[layer], dst_ref=edge_in.at[layer], send_sem=e_send.at[layer],
            recv_sem=e_recv.at[layer], device_id=right, device_id_type=MESH)

        @pl.when(me < n - 1)
        def _():
            edge.start()

        @pl.when(me == 0)
        def _():
            for g in range(groups):
                carried[g, 8 - reach : 8, :] = jnp.zeros((reach, width), jnp.float32)

        @pl.when(me > 0)
        def _():
            edge.wait_recv()
            for g in range(groups):
                carried[g, 8 - reach : 8, :] = edge_in[layer, g]

        for g in range(groups):
            conv = jnp.zeros((rows, width), jnp.float32)
            for tap in range(reach + 1):
                row = taps[layer, tap : tap + 1, own_columns].astype(jnp.float32)
                conv = conv + row * carried[g, 8 - reach + tap : 8 - reach + tap + rows, :]
            acts[mixed_at, g * rows : (g + 1) * rows, own] = (
                gates[g * rows : (g + 1) * rows, :].astype(jnp.float32) * conv).astype(jnp.bfloat16)

        gather(mixed_at, column_place, all_rows, (2, 1))
        serve_until(first + 3)

        if layer == 0:
            own_now = pl.ds(pl.multiple_of(my_tp * block_width + my_grp * width, width), width)
        else:
            own_now = own

        @pl.loop(0, all_rows // chunk)
        def _(c):
            picked = pl.ds(pl.multiple_of(c * chunk, chunk), chunk)
            product = jnp.dot(acts[mixed_at, picked, :], wide[first + 3], preferred_element_type=jnp.float32)
            stream = (acts[now, picked, own_now].astype(jnp.float32) + product).astype(jnp.bfloat16)
            if layer < layers - 1:
                acts[now + 2, picked, own] = stream
            else:
                last[picked, :] = stream

        if layer < layers - 1:
            gather(now + 2, column_place, all_rows, (3, 3))

    mine = pl.ds(pl.multiple_of(my_grp * rows, rows), rows)
    if groups > 1:
        other = lax.rem(my_grp + 1, groups)
        final = pltpu.make_async_remote_copy(
            src_ref=last.at[pl.ds(pl.multiple_of(other * rows, rows), rows), :], dst_ref=swap_in,
            send_sem=r_send, recv_sem=r_recv, device_id=across, device_id_type=MESH)
        final.start()
        result[:, own_columns] = last[mine, :]
        final.wait()
        result[:, pl.ds(pl.multiple_of(other * width, width), width)] = swap_in[...]
    else:
        result[...] = last[...]

    serve(len(queue))
    for c in sends:
        c.wait_send()
    for layer in range(layers):
        @pl.when(me < n - 1)
        def _(layer=layer):
            pltpu.make_async_remote_copy(
                src_ref=edge_out.at[layer], dst_ref=edge_in.at[layer], send_sem=e_send.at[layer],
                recv_sem=e_recv.at[layer], device_id=right, device_id_type=MESH).wait_send()
    for m in range(total):
        for k in range(n):
            @pl.when((me - k >= 0) & (me < n - 1))
            def _(m=m, k=k):
                w_copy(m, me - k, 0).wait_send()

            @pl.when((me + k < n) & (me > 0))
            def _(m=m, k=k):
                w_copy(m, me + k, 1).wait_send()


def shards(tokens, mix_gain, gate_weight, mix_weight, value_weight, out_weight, conv_taps):
    groups, n, tps = lax.axis_size("grp"), lax.axis_size("sp"), lax.axis_size("tp")
    assert groups <= 2
    lows = 2 if tps % 2 == 0 else 1
    highs = tps // lows
    rows, block_width = tokens.shape
    layers, depth, _ = gate_weight.shape
    reach = conv_taps.shape[1] - 1
    width = block_width // groups
    all_rows, features = groups * rows, tps * block_width
    slots = 5 * highs + 3 * highs + 1
    total = layers * KINDS
    anywhere = pl.BlockSpec(memory_space=pl.ANY)
    vmem = pl.BlockSpec(memory_space=pltpu.VMEM)
    dma = pltpu.SemaphoreType.DMA
    return pl.pallas_call(
        functools.partial(kernel, (groups, n, tps, lows)),
        out_shape=jax.ShapeDtypeStruct(tokens.shape, tokens.dtype),
        in_specs=[anywhere, vmem, anywhere, anywhere, anywhere, anywhere, vmem],
        out_specs=vmem,
        scratch_shapes=[
            pltpu.VMEM((total, n * depth, width), jnp.bfloat16),
            pltpu.VMEM((2 * layers, all_rows, features), jnp.bfloat16),
            pltpu.VMEM((groups, rows + 8, width), jnp.float32),
            pltpu.VMEM((all_rows, width), jnp.bfloat16),
            pltpu.VMEM((layers, groups, reach, width), jnp.float32),
            pltpu.VMEM((layers, groups, reach, width), jnp.float32),
            pltpu.VMEM((all_rows, width), jnp.bfloat16),
            pltpu.VMEM((rows, width), jnp.bfloat16),
            dma((total + 1,)),
            dma((total, 2, n)),
            dma((total, n)),
            dma((2 * layers, slots)),
            dma((2 * layers, slots)),
            dma((layers,)),
            dma((layers,)),
            dma,
            dma,
        ],
        compiler_params=pltpu.CompilerParams(
            collective_id=0, has_side_effects=True, vmem_limit_bytes=56 * 1024 * 1024
        ),
        name="mixers",
    )(tokens, mix_gain, gate_weight, mix_weight, value_weight, out_weight, conv_taps)


def solution(mesh):
    return jax.shard_map(
        shards,
        mesh=mesh,
        in_specs=(
            P(("grp", "sp"), "tp"),
            P(),
            P(None, "sp", "tp"),
            P(None, "sp", "tp"),
            P(None, "sp", "tp"),
            P(None, "sp", "tp"),
            P(None, None, "tp"),
        ),
        out_specs=P(("grp", "sp"), "tp"),
        check_vma=False,
    )
```

```python
import functools

import jax
import jax.numpy as jnp
from jax import lax
from jax.experimental import pallas as pl
from jax.experimental.pallas import tpu as pltpu
from jax.sharding import PartitionSpec as P

EPS = 1e-06
KINDS = 4
MESH = pl.DeviceIdType.MESH


def kernel(sizes, tokens, gain, gate_w, mix_w, value_w, out_w, taps, result,
           wide, acts, carried, gates, edge_out, edge_in, last, swap_in,
           local_sem, w_send, w_recv, a_send, a_recv, e_send, e_recv, r_send, r_recv):
    groups, n, tps, lows = sizes
    highs = tps // lows
    rows, block_width = tokens.shape
    layers = gate_w.shape[0]
    depth = gate_w.shape[1]
    width = block_width // groups
    all_rows = groups * rows
    reach = edge_in.shape[2]
    chunk = min(rows, 256)
    me, my_grp, my_tp = lax.axis_index("sp"), lax.axis_index("grp"), lax.axis_index("tp")
    my_high, my_low = my_tp // lows, lax.rem(my_tp, lows)

    def tp_at(high, low):
        return lax.rem(high + highs, highs) * lows + low

    x_next, x_prev = {"tp": tp_at(my_high + 1, my_low)}, {"tp": tp_at(my_high - 1 + highs, my_low)}
    across = {"grp": lax.rem(my_grp + 1, groups)}
    sibling = {"tp": my_high * lows + (1 - my_low)}
    right, left = {"sp": me + 1}, {"sp": me - 1}

    barrier = pltpu.get_barrier_semaphore()
    fixed = []
    if highs > 1:
        fixed.append(x_next)
    if highs > 2:
        fixed.append(x_prev)
    if groups > 1:
        fixed.append(across)
    if lows > 1:
        fixed.append(sibling)
    for device in fixed:
        pl.semaphore_signal(barrier, inc=1, device_id=device, device_id_type=MESH)

    @pl.when(me > 0)
    def _():
        pl.semaphore_signal(barrier, inc=1, device_id=left, device_id_type=MESH)

    @pl.when(me < n - 1)
    def _():
        pl.semaphore_signal(barrier, inc=1, device_id=right, device_id_type=MESH)

    weights = (gate_w, mix_w, value_w, out_w)
    own_columns = pl.ds(pl.multiple_of(my_grp * width, width), width)

    def w_rows(origin):
        return pl.ds(pl.multiple_of(origin * depth, depth), depth)

    def token_place(g, t, offset, size):
        return (pl.ds(pl.multiple_of(g * rows + offset, size), size),
                pl.ds(pl.multiple_of(t * block_width, block_width), block_width))

    def column_place(g, t, offset, size):
        return (pl.ds(offset, size), pl.ds(pl.multiple_of(t * block_width + g * width, width), width))

    own = column_place(my_grp, my_tp, 0, all_rows)[1]
    locals_ = [pltpu.make_async_copy(tokens, acts.at[(0,) + token_place(my_grp, my_tp, 0, rows)], local_sem.at[0])]
    for m in range(layers * KINDS):
        locals_.append(pltpu.make_async_copy(
            weights[m % KINDS].at[m // KINDS, :, own_columns], wide.at[m, w_rows(me), :], local_sem.at[m + 1]))
    for copy in locals_:
        copy.start()
    for copy in locals_:
        copy.wait()

    pl.semaphore_wait(barrier, len(fixed) + jnp.minimum(me, 1) + jnp.minimum(n - 1 - me, 1))

    def w_copy(m, origin, way):
        ref = wide.at[m, w_rows(origin), :]
        return pltpu.make_async_remote_copy(
            src_ref=ref, dst_ref=ref, send_sem=w_send.at[m, way, origin], recv_sem=w_recv.at[m, origin],
            device_id=right if way == 0 else left, device_id_type=MESH)

    def w_own(m):
        @pl.when(me < n - 1)
        def _():
            w_copy(m, me, 0).start()

        @pl.when(me > 0)
        def _():
            w_copy(m, me, 1).start()

    def w_event(m, k):
        @pl.when(me - k >= 0)
        def _():
            w_copy(m, me - k, 0).wait_recv()

            @pl.when(me < n - 1)
            def _():
                w_copy(m, me - k, 0).start()

        @pl.when(me + k < n)
        def _():
            w_copy(m, me + k, 1).wait_recv()

            @pl.when(me > 0)
            def _():
                w_copy(m, me + k, 1).start()

    queue = []
    total = layers * KINDS
    ahead = min(3, total)
    lead = 1 * (n - 1)
    for first in range(0, total, KINDS):
        for part in ((0, 1, 2), (3,)):
            for k in range(1, n):
                for j in part:
                    queue.append((first + j, k))
    state = {"issued": ahead, "done": 0}

    def serve(count):
        while count > 0 and state["done"] < len(queue):
            m, k = queue[state["done"]]
            w_event(m, k)
            state["done"] += 1
            count -= 1
            while state["issued"] < total and queue.index((state["issued"], 1)) <= state["done"] + lead:
                w_own(state["issued"])
                state["issued"] += 1

    def serve_until(m):
        while any(q[0] == m for q in queue[state["done"]:]):
            serve(1)

    sends = []

    def gather(index, sems, place, full):
        half = full // 2
        lane = {"next": 0}

        def copy(origin_grp, origin_tp, offset, size, device, slot):
            ref = acts.at[(index,) + place(origin_grp, origin_tp, offset, size)]
            return pltpu.make_async_remote_copy(
                src_ref=ref, dst_ref=ref, send_sem=a_send.at[sems, slot], recv_sem=a_recv.at[sems, slot],
                device_id=device, device_id_type=MESH)

        def send(g, s, offset, size, device, slot):
            c = copy(lax.rem(my_grp + g, groups), tp_at(my_high - s + highs, my_low), offset, size, device, slot)
            c.start()
            sends.append(c)

        def arrived(g, s, offset, size, slot, low=None):
            low = my_low if low is None else low
            copy(lax.rem(my_grp + g, groups), tp_at(my_high - s + highs, low), offset, size, x_next, slot).wait_recv()

        expected = []

        def to_sibling(g, s, offset, size):
            if lows > 1:
                slot = lane["next"]
                lane["next"] += 1
                send(g, s, offset, size, sibling, slot)
                expected.append((g, s, offset, size, slot))

        x_slot = 5 * highs
        y_slot = x_slot + highs
        top_slot, low_slot = y_slot + 1, y_slot + 1 + highs

        def start():
            if highs > 1:
                send(0, 0, 0, full, x_next, x_slot)
            if groups > 1:
                send(0, 0, 0, full, across, y_slot)
            to_sibling(0, 0, 0, full)

        def turn():
            for s in range(1, highs):
                arrived(0, s, 0, full, x_slot + s - 1)
                if groups > 1:
                    send(0, s, 0, half, across, top_slot + s - 1)
                if s < highs - 1:
                    send(0, s, 0, full, x_next, x_slot + s)
                to_sibling(0, s, 0, full)
            if groups > 1:
                arrived(1, 0, 0, full, y_slot)
                if highs > 1:
                    send(1, 0, half, half, x_next, low_slot)
                to_sibling(1, 0, 0, full)

        def finish():
            if groups > 1:
                for s in range(1, highs):
                    arrived(1, s, half, half, low_slot + s - 1)
                    if s < highs - 1:
                        send(1, s, half, half, x_next, low_slot + s)
                    to_sibling(1, s, half, half)
                    arrived(1, s, 0, half, top_slot + s - 1)
                    to_sibling(1, s, 0, half)
            for g, s, offset, size, slot in expected:
                arrived(g, s, offset, size, slot, 1 - my_low)

        return start, turn, finish

    def part_gather(index, part):
        def place(g, t, offset, size):
            return column_place(g, t, part * rows + offset, size)

        return gather(index, index * groups + part, place, rows)

    parts = range(groups)
    for m in range(ahead):
        w_own(m)
    start, turn, finish = gather(0, 0, token_place, rows)
    start()
    serve(2)
    turn()
    serve(1)
    finish()
    coming = [None] * groups

    chunks = rows // chunk
    for layer in range(layers):
        now, mixed_at = 2 * layer, 2 * layer + 1
        first = layer * KINDS
        for j in range(3):
            serve_until(first + j)

        def project(g, c):
            picked = pl.ds(pl.multiple_of(g * rows + c * chunk, chunk), chunk)
            x = acts[now, picked, :].astype(jnp.float32)
            factor = lax.rsqrt(jnp.mean(x * x, axis=1, keepdims=True) + EPS)
            normed = (x * factor * gain[layer : layer + 1, :].astype(jnp.float32)).astype(jnp.bfloat16)
            gates[picked, :] = jnp.dot(normed, wide[first], preferred_element_type=jnp.float32).astype(jnp.bfloat16)
            inner = jnp.dot(normed, wide[first + 1], preferred_element_type=jnp.float32).astype(jnp.bfloat16)
            values = jnp.dot(normed, wide[first + 2], preferred_element_type=jnp.float32).astype(jnp.bfloat16)
            carried[g, pl.ds(pl.multiple_of(8 + c * chunk, 8), chunk), :] = (
                inner.astype(jnp.float32) * values.astype(jnp.float32))

        def edge(g):
            return pltpu.make_async_remote_copy(
                src_ref=edge_out.at[layer, g], dst_ref=edge_in.at[layer, g], send_sem=e_send.at[layer, g],
                recv_sem=e_recv.at[layer, g], device_id=right, device_id_type=MESH)

        def convolve(g):
            @pl.when(me == 0)
            def _():
                carried[g, 8 - reach : 8, :] = jnp.zeros((reach, width), jnp.float32)

            @pl.when(me > 0)
            def _():
                edge(g).wait_recv()
                carried[g, 8 - reach : 8, :] = edge_in[layer, g]

            conv = jnp.zeros((rows, width), jnp.float32)
            for tap in range(reach + 1):
                row = taps[layer, tap : tap + 1, own_columns].astype(jnp.float32)
                conv = conv + row * carried[g, 8 - reach + tap : 8 - reach + tap + rows, :]
            acts[mixed_at, g * rows : (g + 1) * rows, own] = (
                gates[g * rows : (g + 1) * rows, :].astype(jnp.float32) * conv).astype(jnp.bfloat16)

        going = [part_gather(mixed_at, g) for g in parts]
        for g in parts:
            if coming[g] is not None:
                coming[g][2]()

            @pl.loop(0, chunks)
            def _(i):
                project(g, i)

            edge_out[layer, g] = carried[g, 8 + rows - reach : 8 + rows, :]

            @pl.when(me < n - 1)
            def _():
                edge(g).start()

            if g > 0:
                convolve(g - 1)
                going[g - 1][0]()
        convolve(groups - 1)
        going[groups - 1][0]()

        if layer == 0:
            own_now = pl.ds(pl.multiple_of(my_tp * block_width + my_grp * width, width), width)
        else:
            own_now = own
        coming = [part_gather(now + 2, g) if layer < layers - 1 else None for g in parts]
        for g in parts:
            serve(2)
            going[g][1]()
        serve(1)
        for g in parts:
            going[g][2]()
            serve_until(first + 3)

            @pl.loop(0, chunks)
            def _(c):
                picked = pl.ds(pl.multiple_of(g * rows + c * chunk, chunk), chunk)
                product = jnp.dot(acts[mixed_at, picked, :], wide[first + 3], preferred_element_type=jnp.float32)
                stream = (acts[now, picked, own_now].astype(jnp.float32) + product).astype(jnp.bfloat16)
                if layer < layers - 1:
                    acts[now + 2, picked, own] = stream
                else:
                    last[picked, :] = stream

            if layer < layers - 1:
                coming[g][0]()
        if layer < layers - 1:
            for g in parts:
                serve(2)
                coming[g][1]()
            serve(1)

    mine = pl.ds(pl.multiple_of(my_grp * rows, rows), rows)
    if groups > 1:
        other = lax.rem(my_grp + 1, groups)
        final = pltpu.make_async_remote_copy(
            src_ref=last.at[pl.ds(pl.multiple_of(other * rows, rows), rows), :], dst_ref=swap_in,
            send_sem=r_send, recv_sem=r_recv, device_id=across, device_id_type=MESH)
        final.start()
        result[:, own_columns] = last[mine, :]
        final.wait()
        result[:, pl.ds(pl.multiple_of(other * width, width), width)] = swap_in[...]
    else:
        result[...] = last[...]

    serve(len(queue))
    for c in sends:
        c.wait_send()
    for layer in range(layers):
        for g in parts:
            @pl.when(me < n - 1)
            def _(layer=layer, g=g):
                pltpu.make_async_remote_copy(
                    src_ref=edge_out.at[layer, g], dst_ref=edge_in.at[layer, g], send_sem=e_send.at[layer, g],
                    recv_sem=e_recv.at[layer, g], device_id=right, device_id_type=MESH).wait_send()
    for m in range(total):
        for k in range(n):
            @pl.when((me - k >= 0) & (me < n - 1))
            def _(m=m, k=k):
                w_copy(m, me - k, 0).wait_send()

            @pl.when((me + k < n) & (me > 0))
            def _(m=m, k=k):
                w_copy(m, me + k, 1).wait_send()


def shards(tokens, mix_gain, gate_weight, mix_weight, value_weight, out_weight, conv_taps):
    groups, n, tps = lax.axis_size("grp"), lax.axis_size("sp"), lax.axis_size("tp")
    assert groups <= 2
    lows = 2 if tps % 2 == 0 else 1
    highs = tps // lows
    rows, block_width = tokens.shape
    layers, depth, _ = gate_weight.shape
    reach = conv_taps.shape[1] - 1
    width = block_width // groups
    all_rows, features = groups * rows, tps * block_width
    slots = 5 * highs + 3 * highs + 1
    total = layers * KINDS
    anywhere = pl.BlockSpec(memory_space=pl.ANY)
    vmem = pl.BlockSpec(memory_space=pltpu.VMEM)
    dma = pltpu.SemaphoreType.DMA
    return pl.pallas_call(
        functools.partial(kernel, (groups, n, tps, lows)),
        out_shape=jax.ShapeDtypeStruct(tokens.shape, tokens.dtype),
        in_specs=[anywhere, vmem, anywhere, anywhere, anywhere, anywhere, vmem],
        out_specs=vmem,
        scratch_shapes=[
            pltpu.VMEM((total, n * depth, width), jnp.bfloat16),
            pltpu.VMEM((2 * layers, all_rows, features), jnp.bfloat16),
            pltpu.VMEM((groups, rows + 8, width), jnp.float32),
            pltpu.VMEM((all_rows, width), jnp.bfloat16),
            pltpu.VMEM((layers, groups, reach, width), jnp.float32),
            pltpu.VMEM((layers, groups, reach, width), jnp.float32),
            pltpu.VMEM((all_rows, width), jnp.bfloat16),
            pltpu.VMEM((rows, width), jnp.bfloat16),
            dma((total + 1,)),
            dma((total, 2, n)),
            dma((total, n)),
            dma((2 * layers * groups, slots)),
            dma((2 * layers * groups, slots)),
            dma((layers, groups)),
            dma((layers, groups)),
            dma,
            dma,
        ],
        compiler_params=pltpu.CompilerParams(
            collective_id=0, has_side_effects=True, vmem_limit_bytes=56 * 1024 * 1024
        ),
        name="mixers",
    )(tokens, mix_gain, gate_weight, mix_weight, value_weight, out_weight, conv_taps)


def solution(mesh):
    return jax.shard_map(
        shards,
        mesh=mesh,
        in_specs=(
            P(("grp", "sp"), "tp"),
            P(),
            P(None, "sp", "tp"),
            P(None, "sp", "tp"),
            P(None, "sp", "tp"),
            P(None, "sp", "tp"),
            P(None, None, "tp"),
        ),
        out_specs=P(("grp", "sp"), "tp"),
        check_vma=False,
    )
```

```python
import functools

import jax
import jax.numpy as jnp
from jax import lax
from jax.experimental import pallas as pl
from jax.experimental.pallas import tpu as pltpu
from jax.sharding import PartitionSpec as P

EPS = 1e-06
KINDS = 4
MESH = pl.DeviceIdType.MESH


def kernel(sizes, tokens, gain, gate_w, mix_w, value_w, out_w, taps, result,
           wide, acts, carried, gates, edge_out, edge_in, last, swap_in,
           local_sem, w_send, w_recv, a_send, a_recv, e_send, e_recv, r_send, r_recv):
    groups, n, tps, lows = sizes
    highs = tps // lows
    rows, block_width = tokens.shape
    layers = gate_w.shape[0]
    depth = gate_w.shape[1]
    width = block_width // groups
    all_rows = groups * rows
    reach = edge_in.shape[2]
    chunk = min(rows, 256)
    me, my_grp, my_tp = lax.axis_index("sp"), lax.axis_index("grp"), lax.axis_index("tp")
    my_high, my_low = my_tp // lows, lax.rem(my_tp, lows)

    def tp_at(high, low):
        return lax.rem(high + highs, highs) * lows + low

    x_next, x_prev = {"tp": tp_at(my_high + 1, my_low)}, {"tp": tp_at(my_high - 1 + highs, my_low)}
    across = {"grp": lax.rem(my_grp + 1, groups)}
    sibling = {"tp": my_high * lows + (1 - my_low)}
    right, left = {"sp": me + 1}, {"sp": me - 1}

    barrier = pltpu.get_barrier_semaphore()
    fixed = []
    if highs > 1:
        fixed.append(x_next)
    if highs > 2:
        fixed.append(x_prev)
    if groups > 1:
        fixed.append(across)
    if lows > 1:
        fixed.append(sibling)
    for device in fixed:
        pl.semaphore_signal(barrier, inc=1, device_id=device, device_id_type=MESH)

    @pl.when(me > 0)
    def _():
        pl.semaphore_signal(barrier, inc=1, device_id=left, device_id_type=MESH)

    @pl.when(me < n - 1)
    def _():
        pl.semaphore_signal(barrier, inc=1, device_id=right, device_id_type=MESH)

    weights = (gate_w, mix_w, value_w, out_w)
    own_columns = pl.ds(pl.multiple_of(my_grp * width, width), width)

    def w_rows(origin):
        return pl.ds(pl.multiple_of(origin * depth, depth), depth)

    def token_place(g, t, offset, size):
        return (pl.ds(pl.multiple_of(g * rows + offset, size), size),
                pl.ds(pl.multiple_of(t * block_width, block_width), block_width))

    def column_place(g, t, offset, size):
        return (pl.ds(offset, size), pl.ds(pl.multiple_of(t * block_width + g * width, width), width))

    own = column_place(my_grp, my_tp, 0, all_rows)[1]
    locals_ = [pltpu.make_async_copy(tokens, acts.at[(0,) + token_place(my_grp, my_tp, 0, rows)], local_sem.at[0])]
    for m in range(layers * KINDS):
        locals_.append(pltpu.make_async_copy(
            weights[m % KINDS].at[m // KINDS, :, own_columns], wide.at[m, w_rows(me), :], local_sem.at[m + 1]))
    for copy in locals_:
        copy.start()
    for copy in locals_[:4]:
        copy.wait()

    pl.semaphore_wait(barrier, len(fixed) + jnp.minimum(me, 1) + jnp.minimum(n - 1 - me, 1))

    def w_copy(m, origin, way):
        ref = wide.at[m, w_rows(origin), :]
        return pltpu.make_async_remote_copy(
            src_ref=ref, dst_ref=ref, send_sem=w_send.at[m, way, origin], recv_sem=w_recv.at[m, origin],
            device_id=right if way == 0 else left, device_id_type=MESH)

    def w_own(m):
        @pl.when(me < n - 1)
        def _():
            w_copy(m, me, 0).start()

        @pl.when(me > 0)
        def _():
            w_copy(m, me, 1).start()

    def w_event(m, k):
        @pl.when(me - k >= 0)
        def _():
            w_copy(m, me - k, 0).wait_recv()

            @pl.when(me < n - 1)
            def _():
                w_copy(m, me - k, 0).start()

        @pl.when(me + k < n)
        def _():
            w_copy(m, me + k, 1).wait_recv()

            @pl.when(me > 0)
            def _():
                w_copy(m, me + k, 1).start()

    queue = []
    total = layers * KINDS
    ahead = min(3, total)
    lead = 1 * (n - 1)
    for first in range(0, total, KINDS):
        for part in ((0, 1, 2), (3,)):
            for k in range(1, n):
                for j in part:
                    queue.append((first + j, k))
    state = {"issued": ahead, "done": 0}

    def serve(count):
        while count > 0 and state["done"] < len(queue):
            m, k = queue[state["done"]]
            w_event(m, k)
            state["done"] += 1
            count -= 1
            while state["issued"] < total and queue.index((state["issued"], 1)) <= state["done"] + lead:
                w_own(state["issued"])
                state["issued"] += 1

    def serve_until(m):
        while any(q[0] == m for q in queue[state["done"]:]):
            serve(1)

    sends = []

    def gather(index, sems, place, full):
        half = full // 2
        lane = {"next": 0}

        def copy(origin_grp, origin_tp, offset, size, device, slot):
            ref = acts.at[(index,) + place(origin_grp, origin_tp, offset, size)]
            return pltpu.make_async_remote_copy(
                src_ref=ref, dst_ref=ref, send_sem=a_send.at[sems, slot], recv_sem=a_recv.at[sems, slot],
                device_id=device, device_id_type=MESH)

        def send(g, s, offset, size, device, slot):
            c = copy(lax.rem(my_grp + g, groups), tp_at(my_high - s + highs, my_low), offset, size, device, slot)
            c.start()
            sends.append(c)

        def arrived(g, s, offset, size, slot, low=None):
            low = my_low if low is None else low
            copy(lax.rem(my_grp + g, groups), tp_at(my_high - s + highs, low), offset, size, x_next, slot).wait_recv()

        expected = []

        def to_sibling(g, s, offset, size):
            if lows > 1:
                slot = lane["next"]
                lane["next"] += 1
                send(g, s, offset, size, sibling, slot)
                expected.append((g, s, offset, size, slot))

        x_slot = 5 * highs
        y_slot = x_slot + highs
        top_slot, low_slot = y_slot + 1, y_slot + 1 + highs

        def start():
            if highs > 1:
                send(0, 0, 0, full, x_next, x_slot)
            if groups > 1:
                send(0, 0, 0, full, across, y_slot)
            to_sibling(0, 0, 0, full)

        def turn():
            for s in range(1, highs):
                arrived(0, s, 0, full, x_slot + s - 1)
                if groups > 1:
                    send(0, s, 0, half, across, top_slot + s - 1)
                if s < highs - 1:
                    send(0, s, 0, full, x_next, x_slot + s)
                to_sibling(0, s, 0, full)
            if groups > 1:
                arrived(1, 0, 0, full, y_slot)
                if highs > 1:
                    send(1, 0, half, half, x_next, low_slot)
                to_sibling(1, 0, 0, full)

        def finish():
            if groups > 1:
                for s in range(1, highs):
                    arrived(1, s, half, half, low_slot + s - 1)
                    if s < highs - 1:
                        send(1, s, half, half, x_next, low_slot + s)
                    to_sibling(1, s, half, half)
                    arrived(1, s, 0, half, top_slot + s - 1)
                    to_sibling(1, s, 0, half)
            for g, s, offset, size, slot in expected:
                arrived(g, s, offset, size, slot, 1 - my_low)

        return start, turn, finish

    def part_gather(index, part):
        def place(g, t, offset, size):
            return column_place(g, t, part * rows + offset, size)

        return gather(index, index * groups + part, place, rows)

    parts = range(groups)
    for m in range(ahead):
        w_own(m)
    start, turn, finish = gather(0, 0, token_place, rows)
    start()
    for copy in locals_[4:]:
        copy.wait()
    serve(2)
    turn()
    serve(1)
    finish()
    coming = [None] * groups

    chunks = rows // chunk
    for layer in range(layers):
        now, mixed_at = 2 * layer, 2 * layer + 1
        first = layer * KINDS
        for j in range(3):
            serve_until(first + j)

        def project(g, c):
            picked = pl.ds(pl.multiple_of(g * rows + c * chunk, chunk), chunk)
            x = acts[now, picked, :].astype(jnp.float32)
            factor = lax.rsqrt(jnp.mean(x * x, axis=1, keepdims=True) + EPS)
            normed = (x * factor * gain[layer : layer + 1, :].astype(jnp.float32)).astype(jnp.bfloat16)
            gates[picked, :] = jnp.dot(normed, wide[first], preferred_element_type=jnp.float32).astype(jnp.bfloat16)
            inner = jnp.dot(normed, wide[first + 1], preferred_element_type=jnp.float32).astype(jnp.bfloat16)
            values = jnp.dot(normed, wide[first + 2], preferred_element_type=jnp.float32).astype(jnp.bfloat16)
            carried[g, pl.ds(pl.multiple_of(8 + c * chunk, 8), chunk), :] = (
                inner.astype(jnp.float32) * values.astype(jnp.float32))

        def edge(g):
            return pltpu.make_async_remote_copy(
                src_ref=edge_out.at[layer, g], dst_ref=edge_in.at[layer, g], send_sem=e_send.at[layer, g],
                recv_sem=e_recv.at[layer, g], device_id=right, device_id_type=MESH)

        def convolve(g):
            @pl.when(me == 0)
            def _():
                carried[g, 8 - reach : 8, :] = jnp.zeros((reach, width), jnp.float32)

            @pl.when(me > 0)
            def _():
                edge(g).wait_recv()
                carried[g, 8 - reach : 8, :] = edge_in[layer, g]

            conv = jnp.zeros((rows, width), jnp.float32)
            for tap in range(reach + 1):
                row = taps[layer, tap : tap + 1, own_columns].astype(jnp.float32)
                conv = conv + row * carried[g, 8 - reach + tap : 8 - reach + tap + rows, :]
            acts[mixed_at, g * rows : (g + 1) * rows, own] = (
                gates[g * rows : (g + 1) * rows, :].astype(jnp.float32) * conv).astype(jnp.bfloat16)

        going = [part_gather(mixed_at, g) for g in parts]
        for g in parts:
            if coming[g] is not None:
                coming[g][2]()

            @pl.loop(0, chunks)
            def _(i):
                project(g, i)

            edge_out[layer, g] = carried[g, 8 + rows - reach : 8 + rows, :]

            @pl.when(me < n - 1)
            def _():
                edge(g).start()

            if g > 0:
                convolve(g - 1)
                going[g - 1][0]()
        convolve(groups - 1)
        going[groups - 1][0]()

        if layer == 0:
            own_now = pl.ds(pl.multiple_of(my_tp * block_width + my_grp * width, width), width)
        else:
            own_now = own
        coming = [part_gather(now + 2, g) if layer < layers - 1 else None for g in parts]
        for g in parts:
            serve(2)
            going[g][1]()
        serve(1)
        for g in parts:
            going[g][2]()
            serve_until(first + 3)

            @pl.loop(0, chunks)
            def _(c):
                picked = pl.ds(pl.multiple_of(g * rows + c * chunk, chunk), chunk)
                product = jnp.dot(acts[mixed_at, picked, :], wide[first + 3], preferred_element_type=jnp.float32)
                stream = (acts[now, picked, own_now].astype(jnp.float32) + product).astype(jnp.bfloat16)
                if layer < layers - 1:
                    acts[now + 2, picked, own] = stream
                else:
                    last[picked, :] = stream

            if layer < layers - 1:
                coming[g][0]()
        if layer < layers - 1:
            for g in parts:
                serve(2)
                coming[g][1]()
            serve(1)

    mine = pl.ds(pl.multiple_of(my_grp * rows, rows), rows)
    if groups > 1:
        other = lax.rem(my_grp + 1, groups)
        final = pltpu.make_async_remote_copy(
            src_ref=last.at[pl.ds(pl.multiple_of(other * rows, rows), rows), :], dst_ref=swap_in,
            send_sem=r_send, recv_sem=r_recv, device_id=across, device_id_type=MESH)
        final.start()
        result[:, own_columns] = last[mine, :]
        final.wait()
        result[:, pl.ds(pl.multiple_of(other * width, width), width)] = swap_in[...]
    else:
        result[...] = last[...]

    serve(len(queue))
    for c in sends:
        c.wait_send()
    for layer in range(layers):
        for g in parts:
            @pl.when(me < n - 1)
            def _(layer=layer, g=g):
                pltpu.make_async_remote_copy(
                    src_ref=edge_out.at[layer, g], dst_ref=edge_in.at[layer, g], send_sem=e_send.at[layer, g],
                    recv_sem=e_recv.at[layer, g], device_id=right, device_id_type=MESH).wait_send()
    for m in range(total):
        for k in range(n):
            @pl.when((me - k >= 0) & (me < n - 1))
            def _(m=m, k=k):
                w_copy(m, me - k, 0).wait_send()

            @pl.when((me + k < n) & (me > 0))
            def _(m=m, k=k):
                w_copy(m, me + k, 1).wait_send()


def shards(tokens, mix_gain, gate_weight, mix_weight, value_weight, out_weight, conv_taps):
    groups, n, tps = lax.axis_size("grp"), lax.axis_size("sp"), lax.axis_size("tp")
    assert groups <= 2
    lows = 2 if tps % 2 == 0 else 1
    highs = tps // lows
    rows, block_width = tokens.shape
    layers, depth, _ = gate_weight.shape
    reach = conv_taps.shape[1] - 1
    width = block_width // groups
    all_rows, features = groups * rows, tps * block_width
    slots = 5 * highs + 3 * highs + 1
    total = layers * KINDS
    anywhere = pl.BlockSpec(memory_space=pl.ANY)
    vmem = pl.BlockSpec(memory_space=pltpu.VMEM)
    dma = pltpu.SemaphoreType.DMA
    return pl.pallas_call(
        functools.partial(kernel, (groups, n, tps, lows)),
        out_shape=jax.ShapeDtypeStruct(tokens.shape, tokens.dtype),
        in_specs=[anywhere, vmem, anywhere, anywhere, anywhere, anywhere, vmem],
        out_specs=vmem,
        scratch_shapes=[
            pltpu.VMEM((total, n * depth, width), jnp.bfloat16),
            pltpu.VMEM((2 * layers, all_rows, features), jnp.bfloat16),
            pltpu.VMEM((groups, rows + 8, width), jnp.float32),
            pltpu.VMEM((all_rows, width), jnp.bfloat16),
            pltpu.VMEM((layers, groups, reach, width), jnp.float32),
            pltpu.VMEM((layers, groups, reach, width), jnp.float32),
            pltpu.VMEM((all_rows, width), jnp.bfloat16),
            pltpu.VMEM((rows, width), jnp.bfloat16),
            dma((total + 1,)),
            dma((total, 2, n)),
            dma((total, n)),
            dma((2 * layers * groups, slots)),
            dma((2 * layers * groups, slots)),
            dma((layers, groups)),
            dma((layers, groups)),
            dma,
            dma,
        ],
        compiler_params=pltpu.CompilerParams(
            collective_id=0, has_side_effects=True, vmem_limit_bytes=56 * 1024 * 1024
        ),
        name="mixers",
    )(tokens, mix_gain, gate_weight, mix_weight, value_weight, out_weight, conv_taps)


def solution(mesh):
    return jax.shard_map(
        shards,
        mesh=mesh,
        in_specs=(
            P(("grp", "sp"), "tp"),
            P(),
            P(None, "sp", "tp"),
            P(None, "sp", "tp"),
            P(None, "sp", "tp"),
            P(None, "sp", "tp"),
            P(None, None, "tp"),
        ),
        out_specs=P(("grp", "sp"), "tp"),
        check_vma=False,
    )
```
